32 devices in a mesh: ep: 4 (over y, x), tp: 8 (over z, core).
Axes of the slice: x: 2, y: 2, z: 4, core: 2. Of those that a mesh axis runs over, the one named last changes fastest.
Arguments:
- queries: bfloat16 [4096, 1024], P('ep', 'tp'), may hold values from -6 to 6
- keys: bfloat16 [4096, 256], P('ep'), may hold values from -6 to 6, as said below
- values: bfloat16 [4096, 256], P('ep'), may hold values from -6 to 6
- slopes: float32 [16], P('tp'), may hold values from 0.002 to 0.08
- sinks: float32 [16], P('tp'), may hold values from 2 to 6
- out_weight: bfloat16 [1024, 2048], P('tp'), may hold values from -0.1875 to 0.1875
- mix_gain: float32 [2048], replicated, may hold values from 0.1 to 1.9
- moe_input: bfloat16 [4096, 2048], P(('ep', 'tp')), may hold values from -6 to 6
- in_gain: float32 [2048], replicated, may hold values from 0.1 to 1.9
- out_gain: float32 [2048], replicated, may hold values from 0.1 to 1.9
- group_router: bfloat16 [2048, 4], replicated, may hold values from -0.125 to 0.125
- expert_router: bfloat16 [2048, 4], replicated, may hold values from -0.125 to 0.125
- routes: int32 [4096, 2], P(('ep', 'tp')), may hold values from 0 to 3, all different within a row; in each aligned block of 128 rows (0 to 127, 128 to 255, ...) at most 96 rows name the same one
- gate_weight: bfloat16 [4, 2048, 1024], P('ep', None, 'tp'), may hold values from -0.125 to 0.125
- up_weight: bfloat16 [4, 2048, 1024], P('ep', None, 'tp'), may hold values from -0.125 to 0.125
- down_weight: bfloat16 [4, 2048, 1024], P('ep', None, 'tp'), may hold values from -0.1875 to 0.1875
Outputs:
- mixer_output: bfloat16 [4096, 2048], P(('ep', 'tp'))
- moe_output: bfloat16 [4096, 2048], P(('ep', 'tp'))
The draws below stay inside these ranges and needn't reach their ends.
Inputs may be any that keep to these rules, and one draw needn't show every extreme that they name: `keys`: keys share one value range with the queries. `routes`: A token names 2 different experts. Among the rows of one device no expert is named more than 96 times, a bound that some block reaches in every draw.
All inputs are finite; a program needn't handle non-finite values.
Results may differ from the reference program's by a relative error of at most 0.018.
Values may be sent and summed in bfloat16 or wider, within the bound.
No kernel may reach another device: no remote copies, remote signals or barrier semaphores. Data moves between devices by JAX's collectives and lax.ppermute only.
A program may use at most 128 MiB of HBM per device.

```python
import math
import jax
import jax.numpy as jnp
import numpy as np
from jax import lax

D = 2048
HEADS = 16
HD = 64
KV_HEADS = 4
WINDOW = 128
DE = 1024
GROUPS = 4
TOP = 2
TOK_DEV = 128
EXPERTS = 4
CAP = 96
TOKENS = 4096
N_TP = 8


def draw_keys(key, part):
    drawn = jnp.clip(jax.random.normal(jax.random.fold_in(key, 3), (TOKENS, KV_HEADS, HD), jnp.float32), -5.9, 5.9)
    return drawn.reshape(TOKENS, KV_HEADS * HD).astype(jnp.bfloat16)


def draw_queries(key, part):
    drawn = jnp.clip(jax.random.normal(jax.random.fold_in(key, 4), (TOKENS, HEADS, HD), jnp.float32), -5.9, 5.9)
    return drawn.reshape(TOKENS, HEADS * HD).astype(jnp.bfloat16)


def block_scale(rng, shape, shards, smallest, top_value):
    level = 1.0
    for dim, blocks in shards:
        heights = jax.random.uniform(jax.random.fold_in(jax.random.fold_in(rng, 6), dim), (blocks,), jnp.float32, smallest / len(shards), top_value / len(shards))
        level = level * jnp.repeat(jnp.exp(heights), shape[dim] // blocks).reshape((-1,) + (1,) * (len(shape) - 1 - dim))
    return level


def assign_block(key, own, number, rows, amount, top, reach, skew):
    sequence = jax.random.permutation(key, amount)
    heavy_load, common = portions_of(amount, rows * top, reach, skew, True), portions_of(amount, rows * top, reach, skew, False)
    places = jnp.arange(amount)

    def named(sizes, rotation):
        used = int((sizes > 0).sum())
        fixed = max(1, used // 4)
        passed = fixed + (places - fixed + rotation * (used - fixed)) % max(1, amount - fixed)
        return jnp.zeros((amount,), jnp.int32).at[sequence[jnp.where(places < fixed, places, passed)]].set(jnp.asarray(sizes, jnp.int32))

    sizes = jnp.where(number % 4 == 0, named(heavy_load, number // 4), named(common, number - number // 4 - 1))
    mixed = jax.random.permutation(jax.random.fold_in(own, 3), amount)
    giver, receiver = mixed[0:amount // 2 * 2:2], mixed[1:amount // 2 * 2:2]
    slack = jnp.minimum(sizes[giver] - 1, reach - sizes[receiver]) // 2
    slack = jnp.where((giver == sequence[0]) | (receiver == sequence[0]) | (sizes[receiver] == 0), 0, jnp.maximum(slack, 0))
    passed = jax.random.randint(jax.random.fold_in(own, 4), (amount // 2,), 0, 1 << 20) % (slack + 1)
    sizes = sizes.at[giver].add(-passed).at[receiver].add(passed)
    items = jnp.searchsorted(jnp.cumsum(sizes), jnp.arange(rows * top), side="right").astype(jnp.int32)
    listing = items.reshape(top, rows).T
    listing = listing[jax.random.permutation(jax.random.fold_in(own, 1), rows)]
    rotation = jax.random.randint(jax.random.fold_in(own, 2), (rows, 1), 0, top)
    return jnp.take_along_axis(listing, (jnp.arange(top)[None, :] + rotation) % top, axis=1)


def portions_of(count, total, reach, slope, full):
    loads = [(1 << 20) // math.isqrt(standing ** slope) + 1 for standing in range(1, count + 1)]
    largest = reach if full else min(reach, max(-(-total // count), total * loads[0] // sum(loads)))
    least = 1 if total - largest >= count - 1 else 0
    counts, rest = [largest] + [least] * (count - 1), total - largest - least * (count - 1)
    while rest > 0:
        free = [i for i in range(1, count) if counts[i] < largest] or [i for i in range(1, count) if counts[i] < reach]
        whole, left = sum([loads[i] for i in free]), rest
        for i in free:
            more = min(reach - counts[i], max(1, left * loads[i] // whole), rest)
            counts[i] = counts[i] + more
            rest = rest - more
    return np.array(counts)


def noise(stream_key, shape, spread, reach, pieces=(), kind=jnp.bfloat16):
    result = jax.random.normal(stream_key, shape, jnp.float32) * spread
    if len(pieces) > 0:
        result = block_scale(stream_key, shape, pieces, -0.22, 0.18) * result
    return jnp.clip(result, min=-reach, max=reach).astype(kind)


def setup_inputs(seed: int = 0) -> dict:
    arg_keys = jax.random.split(jax.random.key(seed), 17)
    queries = draw_queries(jax.random.fold_in(arg_keys[16], 71), 0)
    keys = draw_keys(jax.random.fold_in(arg_keys[16], 71), 0)
    values = noise(arg_keys[2], (TOKENS, KV_HEADS * HD), 1.0, 6.0, ((0, 4),))
    slopes = jnp.clip(jnp.exp(math.log(0.08) - 3.6888794 * jax.random.uniform(arg_keys[3], (HEADS,), jnp.float32) ** block_scale(arg_keys[3], (HEADS,), ((0, 8),), -0.2, 0.2)), 0.002, 0.08)
    sinks = jnp.clip(2.0 + 4.0 * jax.random.uniform(arg_keys[4], (HEADS,), jnp.float32) ** block_scale(arg_keys[4], (HEADS,), ((0, 8),), -0.2, 0.2), 2.0, 6.0)
    out_weight = noise(arg_keys[5], (HEADS * HD, D), (HEADS * HD) ** -0.5, 0.1875, ((0, 8),))
    mix_gain = jnp.clip(1.0 + 0.18 * jax.random.normal(arg_keys[6], (D,), jnp.float32), 0.1, 1.9)
    moe_input = noise(arg_keys[7], (TOKENS, D), 1.0, 6.0, ((0, 32),))
    in_gain = jnp.clip(1.0 + 0.18 * jax.random.normal(arg_keys[8], (D,), jnp.float32), 0.1, 1.9)
    out_gain = jnp.clip(1.0 + 0.18 * jax.random.normal(arg_keys[9], (D,), jnp.float32), 0.1, 1.9)
    group_router = noise(arg_keys[10], (D, GROUPS), D ** -0.5, 0.125)
    expert_router = noise(arg_keys[11], (D, EXPERTS), D ** -0.5, 0.125)
    routes_keys = jax.random.split(jax.random.fold_in(arg_keys[12], 1), TOKENS // TOK_DEV)
    routes_turns = jax.random.permutation(jax.random.fold_in(arg_keys[12], 3), TOKENS // TOK_DEV)
    routes = jax.vmap(lambda own, number: assign_block(jax.random.fold_in(arg_keys[12], 2), own, number, TOK_DEV, EXPERTS, TOP, CAP, 2))(routes_keys, routes_turns).reshape((TOKENS, TOP))
    gate_weight = noise(arg_keys[13], (EXPERTS, D, DE), D ** -0.5, 0.125, ((0, 4), (2, 8)))
    up_weight = noise(arg_keys[14], (EXPERTS, D, DE), D ** -0.5, 0.125, ((0, 4), (2, 8)))
    down_weight = noise(arg_keys[15], (EXPERTS, D, DE), DE ** -0.5, 0.1875, ((0, 4), (2, 8)))
    return dict(queries=queries, keys=keys, values=values, slopes=slopes, sinks=sinks, out_weight=out_weight, mix_gain=mix_gain, moe_input=moe_input, in_gain=in_gain, out_gain=out_gain, group_router=group_router, expert_router=expert_router, routes=routes, gate_weight=gate_weight, up_weight=up_weight, down_weight=down_weight)


eps = 1e-06

def scale_rows(matrix, gain):
    mean_square = lax.optimization_barrier(jnp.mean(matrix * matrix, axis=-1, keepdims=True))
    return matrix * lax.rsqrt(mean_square + eps) * gain

def attend(queries, keys, values, slopes, sinks):
    per_kv = HEADS // KV_HEADS
    blocks = TOKENS // WINDOW
    query_blocks = queries.astype(jnp.float32).reshape(blocks, WINDOW, KV_HEADS, per_kv, HD)
    key_blocks = keys.astype(jnp.float32).reshape(blocks, WINDOW, KV_HEADS, HD)
    value_blocks = values.astype(jnp.float32).reshape(blocks, WINDOW, KV_HEADS, HD)
    empty = jnp.zeros((1, WINDOW, KV_HEADS, HD), jnp.float32)
    key_span = jnp.concatenate([jnp.concatenate([empty, key_blocks[:-1]], axis=0), key_blocks], axis=1)
    value_span = jnp.concatenate([jnp.concatenate([empty, value_blocks[:-1]], axis=0), value_blocks], axis=1)
    scores = jnp.einsum('nqkgd,nskd->nkgqs', query_blocks, key_span) * (1.0 / math.sqrt(HD))
    query_index = jnp.arange(WINDOW, dtype=jnp.int32)[:, None]
    key_index = jnp.arange(2 * WINDOW, dtype=jnp.int32)[None, :]
    distance = query_index + WINDOW - key_index
    key_position = jnp.arange(blocks, dtype=jnp.int32)[:, None, None] * WINDOW + key_index[None] - WINDOW
    valid = ((distance >= 0) & (distance < WINDOW))[None] & (key_position >= 0)
    slope_table = slopes.reshape(KV_HEADS, per_kv)
    scores = scores - slope_table[None, :, :, None, None] * distance.astype(jnp.float32)[None, None, None]
    scores = jnp.where(valid[:, None, None], scores, -jnp.inf)
    sink = sinks.reshape(KV_HEADS, per_kv)[None, :, :, None, None]
    top = jnp.maximum(lax.optimization_barrier(jnp.max(scores, axis=-1, keepdims=True)), sink)
    weights = jnp.exp(scores - top)
    denom = lax.optimization_barrier(jnp.sum(weights, axis=-1, keepdims=True)) + jnp.exp(sink - top)
    probs = (weights / denom).astype(jnp.bfloat16)
    attention = jnp.einsum('nkgqs,nskd->nqkgd', probs.astype(jnp.float32), value_span)
    return attention.astype(jnp.bfloat16).reshape(TOKENS, HEADS * HD)

def reference(queries, keys, values, slopes, sinks, out_weight, mix_gain, moe_input, in_gain, out_gain, group_router, expert_router, routes, gate_weight, up_weight, down_weight):
    attention = attend(queries, keys, values, slopes, sinks)
    shard = HEADS * HD // N_TP
    projected = jnp.zeros((TOKENS, D), jnp.float32)
    for shard_index in range(N_TP):
        lower = shard_index * shard
        part = jnp.dot(attention[:, lower:lower + shard], out_weight[lower:lower + shard], preferred_element_type=jnp.float32)
        rounded = lax.optimization_barrier(part.astype(jnp.bfloat16))
        projected = projected + rounded.astype(jnp.float32)
    mixer_output = scale_rows(projected, mix_gain).astype(jnp.bfloat16)
    normed = scale_rows(moe_input.astype(jnp.float32), in_gain).astype(jnp.bfloat16)
    group_logits = jnp.dot(normed, group_router, preferred_element_type=jnp.float32)
    expert_logits = jnp.dot(normed, expert_router, preferred_element_type=jnp.float32)
    per_group = EXPERTS // GROUPS
    expert_match = routes[:, :, None] == jnp.arange(EXPERTS, dtype=jnp.int32)[None, None, :]
    picked_logits = lax.optimization_barrier(jnp.sum(jnp.where(expert_match, expert_logits[:, None, :], 0.0), axis=-1))
    group_prob = jax.nn.softmax(group_logits, axis=-1)
    group_match = (routes // per_group)[:, :, None] == jnp.arange(GROUPS, dtype=jnp.int32)[None, None, :]
    picked_group = lax.optimization_barrier(jnp.sum(jnp.where(group_match, group_prob[:, None, :], 0.0), axis=-1))
    route_weight = picked_group * jax.nn.softmax(picked_logits, axis=-1)
    blocks = TOKENS // TOK_DEV
    match_int = expert_match.astype(jnp.int32).reshape(blocks, TOK_DEV * TOP, EXPERTS)
    before = jnp.cumsum(match_int, axis=1) - match_int
    slot = lax.optimization_barrier(jnp.sum(before * match_int, axis=-1)).reshape(TOKENS, TOP)
    block_of = (jnp.arange(TOKENS, dtype=jnp.int32) // TOK_DEV)[:, None]
    column = (block_of * CAP + slot).astype(jnp.int32)
    token_ids = jnp.broadcast_to(jnp.arange(TOKENS, dtype=jnp.int32)[:, None], (TOKENS, TOP))
    table = jnp.full((EXPERTS, blocks * CAP), TOKENS, jnp.int32)
    table = table.at[routes.reshape(-1), column.reshape(-1)].set(token_ids.reshape(-1))
    weight_table = jnp.zeros((EXPERTS, blocks * CAP), jnp.float32)
    weight_table = weight_table.at[routes.reshape(-1), column.reshape(-1)].set(route_weight.reshape(-1))
    padded = jnp.concatenate([normed, jnp.zeros((1, D), normed.dtype)], axis=0)

    def one_expert(running, expert):
        index = table[expert]
        rows = jnp.take(padded, index, axis=0)
        gate = jnp.dot(rows, gate_weight[expert], preferred_element_type=jnp.float32)
        up = jnp.dot(rows, up_weight[expert], preferred_element_type=jnp.float32)
        hidden = (jax.nn.silu(gate) * up).astype(jnp.bfloat16)
        expert_rows = jnp.dot(hidden, down_weight[expert].T, preferred_element_type=jnp.float32).astype(jnp.bfloat16)
        weighted = weight_table[expert][:, None] * expert_rows.astype(jnp.float32)
        return (running.at[index].add(weighted, mode='drop'), None)
    moe, unused = lax.scan(one_expert, jnp.zeros((TOKENS, D), jnp.float32), jnp.arange(EXPERTS, dtype=jnp.int32))
    moe_output = scale_rows(moe, out_gain).astype(jnp.bfloat16)
    return (mixer_output, moe_output)
```

```python
import math

import jax
import jax.numpy as jnp
from jax import lax
from jax.sharding import PartitionSpec as P

HEADS = 16
HD = 64
KV_HEADS = 4
WINDOW = 128
DOWN_PARTS = 2


eps = 1e-06


def shifted(block, axis, distance):
    devices = range(lax.axis_size(axis))
    route = [(i - distance, i) for i in devices if i - distance in devices]
    return lax.ppermute(block, axis, route)


def swapped(block, axis):
    devices = range(lax.axis_size(axis))
    return lax.ppermute(block, axis, [(i, i ^ 1) for i in devices])


def ring(block, axis, stride):
    count = lax.axis_size(axis)
    route = [(i, (i + stride) % count) for i in range(count)]
    pieces = [block]
    for _ in range(count // stride - 1):
        pieces.append(lax.ppermute(pieces[-1], axis, route))
    return pieces


def offsets(block, axis):
    count = lax.axis_size(axis)
    pieces = [block]
    for step in range(1, count):
        pieces.append(lax.ppermute(block, axis, [(i, i ^ step) for i in range(count)]))
    return pieces


def scale_rows(matrix, gain):
    mean_square = jnp.mean(matrix * matrix, axis=-1, keepdims=True)
    return matrix * lax.rsqrt(mean_square + eps) * gain


def per_device(
    queries,
    keys,
    values,
    slopes,
    sinks,
    out_weight,
    mix_gain,
    moe_input,
    in_gain,
    out_gain,
    group_router,
    expert_router,
    routes,
    gate_weight,
    up_weight,
    down_weight,
):
    rows_group = queries.shape[0]
    local_heads = slopes.shape[0]
    per_kv = HEADS // KV_HEADS
    kv_index = lax.axis_index("tp") * local_heads // per_kv
    own_keys = lax.dynamic_slice_in_dim(keys, kv_index * HD, HD, 1)
    own_values = lax.dynamic_slice_in_dim(values, kv_index * HD, HD, 1)
    rim_keys, rim_values = shifted(
        (own_keys[rows_group - WINDOW :], own_values[rows_group - WINDOW :]), "ep", 1
    )
    blocks = rows_group // WINDOW
    key_blocks = own_keys.reshape(blocks, WINDOW, HD)
    value_blocks = own_values.reshape(blocks, WINDOW, HD)
    key_span = jnp.concatenate(
        [jnp.concatenate([rim_keys[None], key_blocks[:-1]], axis=0), key_blocks], axis=1
    )
    value_span = jnp.concatenate(
        [jnp.concatenate([rim_values[None], value_blocks[:-1]], axis=0), value_blocks], axis=1
    )
    query_blocks = queries.reshape(blocks, WINDOW, local_heads, HD)
    scores = jnp.einsum(
        "nqhd,nsd->nhqs", query_blocks, key_span, preferred_element_type=jnp.float32
    ) * (1.0 / math.sqrt(HD))
    query_index = jnp.arange(WINDOW, dtype=jnp.int32)[:, None]
    key_index = jnp.arange(2 * WINDOW, dtype=jnp.int32)[None, :]
    distance = query_index + WINDOW - key_index
    key_position = (
        lax.axis_index("ep") * rows_group
        + jnp.arange(blocks, dtype=jnp.int32)[:, None, None] * WINDOW
        + key_index[None]
        - WINDOW
    )
    valid = ((distance >= 0) & (distance < WINDOW))[None] & (key_position >= 0)
    scores = scores - slopes[None, :, None, None] * distance.astype(jnp.float32)[None, None]
    scores = jnp.where(valid[:, None], scores, -jnp.inf)
    sink = sinks[None, :, None, None]
    top = jnp.maximum(jnp.max(scores, axis=-1, keepdims=True), sink)
    weights = jnp.exp(scores - top)
    denom = jnp.sum(weights, axis=-1, keepdims=True) + jnp.exp(sink - top)
    probs = (weights / denom).astype(jnp.bfloat16)
    attention = jnp.einsum("nhqs,nsd->nqhd", probs, value_span, preferred_element_type=jnp.float32)
    attention = attention.astype(jnp.bfloat16).reshape(rows_group, local_heads * HD)
    own_rows = moe_input.shape[0]
    ep_size = lax.axis_size("ep")
    tp_size = lax.axis_size("tp")
    ep_index = lax.axis_index("ep")
    core = lax.axis_index("tp") % 2
    width = out_weight.shape[1]
    slab = out_weight.shape[0] // ep_size
    own_slab = lax.dynamic_slice_in_dim(out_weight, ep_index * slab, slab, 0)
    slabs = lax.all_gather(own_slab, "tp", axis=0, tiled=True)
    half_slabs = lax.dynamic_slice_in_dim(slabs, core * (width // 2), width // 2, 1)
    own_half = jnp.stack(offsets(half_slabs, "ep"))
    other_half = swapped(own_half, "tp")
    attention_rows = lax.all_to_all(attention, "tp", split_axis=0, concat_axis=1, tiled=True)
    by_slab = attention_rows.reshape(own_rows, tp_size, ep_size, slab).transpose(2, 0, 1, 3)
    by_slab = by_slab.reshape(ep_size, own_rows, tp_size * slab)
    order = jnp.bitwise_xor(jnp.arange(ep_size, dtype=jnp.int32), ep_index)
    by_slab = jnp.take(by_slab, order, axis=0)
    own_part = jnp.einsum("etk,ekd->td", by_slab, own_half, preferred_element_type=jnp.float32)
    other_part = jnp.einsum("etk,ekd->td", by_slab, other_half, preferred_element_type=jnp.float32)
    projected = jnp.where(
        core == 0,
        jnp.concatenate([own_part, other_part], axis=1),
        jnp.concatenate([other_part, own_part], axis=1),
    )
    mixer_output = scale_rows(projected, mix_gain).astype(jnp.bfloat16)
    normed = scale_rows(moe_input.astype(jnp.float32), in_gain).astype(jnp.bfloat16)
    group_logits = jnp.dot(normed, group_router, preferred_element_type=jnp.float32)
    expert_logits = jnp.dot(normed, expert_router, preferred_element_type=jnp.float32)
    experts = expert_router.shape[1]
    groups = group_router.shape[1]
    per_group = experts // groups
    visits = routes.shape[1]
    expert_match = routes[:, :, None] == jnp.arange(experts, dtype=jnp.int32)[None, None, :]
    picked_logits = jnp.sum(jnp.where(expert_match, expert_logits[:, None, :], 0.0), axis=-1)
    group_prob = jax.nn.softmax(group_logits, axis=-1)
    group_match = (routes // per_group)[:, :, None] == jnp.arange(groups, dtype=jnp.int32)[
        None, None, :
    ]
    picked_group = jnp.sum(jnp.where(group_match, group_prob[:, None, :], 0.0), axis=-1)
    route_weight = picked_group * jax.nn.softmax(picked_logits, axis=-1)
    capacity = max(2, 3 * own_rows * visits // (2 * experts))
    match_int = expert_match.astype(jnp.int32).reshape(own_rows * visits, experts)
    before = jnp.cumsum(match_int, axis=0) - match_int
    slot = jnp.sum(before * match_int, axis=-1)
    position = (routes.reshape(-1) * capacity + slot).reshape(own_rows, visits)
    slot_ids = jnp.arange(experts * capacity, dtype=jnp.int32)
    placement = jnp.any(position[None, :, :] == slot_ids[:, None, None], axis=-1).astype(
        jnp.bfloat16
    )
    outgoing = jnp.dot(placement, normed, preferred_element_type=jnp.float32).astype(jnp.bfloat16)
    local_experts = gate_weight.shape[0]
    outgoing = outgoing.reshape(lax.axis_size("ep"), local_experts, capacity, normed.shape[1])
    arrived = lax.all_to_all(outgoing, "ep", split_axis=0, concat_axis=0, tiled=True)
    rows = ep_size * capacity
    own_arrived = arrived.transpose(1, 0, 2, 3).reshape(local_experts, rows, width)
    both = jnp.concatenate([own_arrived, swapped(own_arrived, "tp")], axis=1)
    units = gate_weight.shape[2]
    gate_up = ring(jnp.concatenate([gate_weight, up_weight], axis=2), "tp", 2)
    hidden_pieces = []
    for piece in gate_up:
        both_gate_up = jnp.einsum("xcd,xdf->xcf", both, piece, preferred_element_type=jnp.float32)
        gate, up = both_gate_up[:, :, :units], both_gate_up[:, :, units:]
        hidden_pieces.append((jax.nn.silu(gate) * up).astype(jnp.bfloat16))
    hidden = jnp.concatenate(hidden_pieces, axis=2)
    picks = [
        (position[:, k][:, None] == slot_ids[None, :]).astype(jnp.bfloat16) for k in range(visits)
    ]
    moe_parts = []
    for down_part in jnp.split(down_weight, DOWN_PARTS, axis=1):
        down_piece = jnp.concatenate(ring(down_part, "tp", 2), axis=2)
        results = jnp.einsum("xcf,xdf->xcd", hidden, down_piece, preferred_element_type=jnp.float32)
        from_other = swapped(results[:, rows:].astype(jnp.bfloat16), "tp")
        summed = (results[:, :rows] + from_other.astype(jnp.float32)).astype(jnp.bfloat16)
        summed = summed.reshape(local_experts, ep_size, capacity, -1).transpose(1, 0, 2, 3)
        returned = lax.all_to_all(summed, "ep", split_axis=0, concat_axis=0, tiled=True)
        flat_back = returned.reshape(experts * capacity, returned.shape[3])
        moe_parts.append(
            sum(
                route_weight[:, k][:, None]
                * jnp.dot(picks[k], flat_back, preferred_element_type=jnp.float32)
                for k in range(visits)
            )
        )
    moe = jnp.concatenate(moe_parts, axis=1)
    moe_output = scale_rows(moe, out_gain).astype(jnp.bfloat16)
    return (mixer_output, moe_output)


def solution(mesh):
    return jax.shard_map(
        per_device,
        mesh=mesh,
        in_specs=(
            P("ep", "tp"),
            P("ep", None),
            P("ep", None),
            P("tp"),
            P("tp"),
            P("tp", None),
            P(),
            P(("ep", "tp"), None),
            P(),
            P(),
            P(),
            P(),
            P(("ep", "tp"), None),
            P("ep", None, "tp"),
            P("ep", None, "tp"),
            P("ep", None, "tp"),
        ),
        out_specs=(P(("ep", "tp"), None), P(("ep", "tp"), None)),
        check_vma=False,
    )
```

```python
import math

import jax
import jax.numpy as jnp
from jax import lax
from jax.sharding import PartitionSpec as P

HEADS = 16
HD = 64
KV_HEADS = 4
WINDOW = 128
DOWN_PARTS = 2


eps = 1e-06


def shifted(block, axis, distance):
    devices = range(lax.axis_size(axis))
    route = [(i - distance, i) for i in devices if i - distance in devices]
    return lax.ppermute(block, axis, route)


def swapped(block, axis):
    devices = range(lax.axis_size(axis))
    return lax.ppermute(block, axis, [(i, i ^ 1) for i in devices])


def offsets(block, axis):
    count = lax.axis_size(axis)
    pieces = [block]
    for step in range(1, count):
        pieces.append(lax.ppermute(block, axis, [(i, i ^ step) for i in range(count)]))
    return pieces


def scale_rows(matrix, gain):
    mean_square = jnp.mean(matrix * matrix, axis=-1, keepdims=True)
    return matrix * lax.rsqrt(mean_square + eps) * gain


def per_device(
    queries,
    keys,
    values,
    slopes,
    sinks,
    out_weight,
    mix_gain,
    moe_input,
    in_gain,
    out_gain,
    group_router,
    expert_router,
    routes,
    gate_weight,
    up_weight,
    down_weight,
):
    tp_size = lax.axis_size("tp")
    ep_size = lax.axis_size("ep")
    ep_index = lax.axis_index("ep")
    slab = out_weight.shape[0] // ep_size
    own_slab = lax.dynamic_slice_in_dim(out_weight, ep_index * slab, slab, 0)
    gate_up_own = jnp.concatenate([gate_weight, up_weight], axis=2)
    slabs = [own_slab]
    for step in range(1, tp_size // 2):
        away = [(i, (i + 2 * step) % tp_size) for i in range(tp_size)]
        slabs.append(lax.ppermute(own_slab, "tp", away))
    z_slabs = jnp.stack(slabs)
    own_slabs = jnp.stack(offsets(z_slabs, "ep"))
    other_slabs = swapped(own_slabs, "tp")
    gate_up, down = [gate_up_own], [down_weight]
    route = [(i, (i + 2) % tp_size) for i in range(tp_size)]
    for _ in range(tp_size // 2 - 1):
        down.append(lax.ppermute(down[-1], "tp", route))
        gate_up.append(lax.ppermute(gate_up[-1], "tp", route))
    rows_group = queries.shape[0]
    local_heads = slopes.shape[0]
    per_kv = HEADS // KV_HEADS
    kv_index = lax.axis_index("tp") * local_heads // per_kv
    own_keys = lax.dynamic_slice_in_dim(keys, kv_index * HD, HD, 1)
    own_values = lax.dynamic_slice_in_dim(values, kv_index * HD, HD, 1)
    own_pairs = jnp.concatenate([own_keys, own_values], axis=1)
    rim = shifted(own_pairs[rows_group - WINDOW :], "ep", 1)
    rim_keys, rim_values = rim[:, :HD], rim[:, HD:]
    blocks = rows_group // WINDOW
    key_blocks = own_keys.reshape(blocks, WINDOW, HD)
    value_blocks = own_values.reshape(blocks, WINDOW, HD)
    key_span = jnp.concatenate(
        [jnp.concatenate([rim_keys[None], key_blocks[:-1]], axis=0), key_blocks], axis=1
    )
    value_span = jnp.concatenate(
        [jnp.concatenate([rim_values[None], value_blocks[:-1]], axis=0), value_blocks], axis=1
    )
    query_blocks = queries.reshape(blocks, WINDOW, local_heads, HD)
    scores = jnp.einsum(
        "nqhd,nsd->nhqs", query_blocks, key_span, preferred_element_type=jnp.float32
    ) * (1.0 / math.sqrt(HD))
    query_index = jnp.arange(WINDOW, dtype=jnp.int32)[:, None]
    key_index = jnp.arange(2 * WINDOW, dtype=jnp.int32)[None, :]
    distance = query_index + WINDOW - key_index
    key_position = (
        lax.axis_index("ep") * rows_group
        + jnp.arange(blocks, dtype=jnp.int32)[:, None, None] * WINDOW
        + key_index[None]
        - WINDOW
    )
    valid = ((distance >= 0) & (distance < WINDOW))[None] & (key_position >= 0)
    scores = scores - slopes[None, :, None, None] * distance.astype(jnp.float32)[None, None]
    scores = jnp.where(valid[:, None], scores, -jnp.inf)
    sink = sinks[None, :, None, None]
    top = jnp.maximum(jnp.max(scores, axis=-1, keepdims=True), sink)
    weights = jnp.exp(scores - top)
    denom = jnp.sum(weights, axis=-1, keepdims=True) + jnp.exp(sink - top)
    probs = (weights / denom).astype(jnp.bfloat16)
    attention = jnp.einsum("nhqs,nsd->nqhd", probs, value_span, preferred_element_type=jnp.float32)
    attention = attention.astype(jnp.bfloat16).reshape(rows_group, local_heads * HD)
    own_rows = moe_input.shape[0]
    core = lax.axis_index("tp") % 2
    width = out_weight.shape[1]
    attention_rows = lax.all_to_all(attention, "tp", split_axis=0, concat_axis=1, tiled=True)
    z_size = tp_size // 2
    by_slab = attention_rows.reshape(own_rows, z_size, 2, ep_size, slab)
    z_order = (lax.axis_index("tp") // 2 - jnp.arange(z_size, dtype=jnp.int32)) % z_size
    ep_order = jnp.bitwise_xor(jnp.arange(ep_size, dtype=jnp.int32), ep_index)
    by_slab = jnp.take(jnp.take(by_slab, z_order, axis=1), ep_order, axis=3)
    by_slab = by_slab.transpose(2, 0, 3, 1, 4).reshape(2, own_rows, ep_size * z_size * slab)
    by_slab = jnp.where(core == 0, by_slab, by_slab[::-1])
    projected = jnp.dot(
        by_slab[0], own_slabs.reshape(-1, width), preferred_element_type=jnp.float32
    ) + jnp.dot(by_slab[1], other_slabs.reshape(-1, width), preferred_element_type=jnp.float32)
    mixer_output = scale_rows(projected, mix_gain).astype(jnp.bfloat16)
    normed = scale_rows(moe_input.astype(jnp.float32), in_gain).astype(jnp.bfloat16)
    group_logits = jnp.dot(normed, group_router, preferred_element_type=jnp.float32)
    expert_logits = jnp.dot(normed, expert_router, preferred_element_type=jnp.float32)
    experts = expert_router.shape[1]
    groups = group_router.shape[1]
    per_group = experts // groups
    visits = routes.shape[1]
    expert_match = routes[:, :, None] == jnp.arange(experts, dtype=jnp.int32)[None, None, :]
    picked_logits = jnp.sum(jnp.where(expert_match, expert_logits[:, None, :], 0.0), axis=-1)
    group_prob = jax.nn.softmax(group_logits, axis=-1)
    group_match = (routes // per_group)[:, :, None] == jnp.arange(groups, dtype=jnp.int32)[
        None, None, :
    ]
    picked_group = jnp.sum(jnp.where(group_match, group_prob[:, None, :], 0.0), axis=-1)
    route_weight = picked_group * jax.nn.softmax(picked_logits, axis=-1)
    capacity = max(2, 3 * own_rows * visits // (2 * experts))
    match_int = expert_match.astype(jnp.int32).reshape(own_rows * visits, experts)
    before = jnp.cumsum(match_int, axis=0) - match_int
    slot = jnp.sum(before * match_int, axis=-1)
    position = (routes.reshape(-1) * capacity + slot).reshape(own_rows, visits)
    slot_ids = jnp.arange(experts * capacity, dtype=jnp.int32)
    placement = jnp.any(position[None, :, :] == slot_ids[:, None, None], axis=-1).astype(
        jnp.bfloat16
    )
    outgoing = jnp.dot(placement, normed, preferred_element_type=jnp.float32).astype(jnp.bfloat16)
    local_experts = gate_weight.shape[0]
    outgoing = outgoing.reshape(lax.axis_size("ep"), local_experts, capacity, normed.shape[1])
    arrived = lax.all_to_all(outgoing, "ep", split_axis=0, concat_axis=0, tiled=True)
    rows = ep_size * capacity
    own_arrived = arrived.transpose(1, 0, 2, 3).reshape(local_experts, rows, width)
    both = jnp.concatenate([own_arrived, swapped(own_arrived, "tp")], axis=1)
    units = gate_weight.shape[2]
    hidden_pieces = []
    for piece in gate_up:
        both_gate_up = jnp.einsum("xcd,xdf->xcf", both, piece, preferred_element_type=jnp.float32)
        gate, up = both_gate_up[:, :, :units], both_gate_up[:, :, units:]
        hidden_pieces.append((jax.nn.silu(gate) * up).astype(jnp.bfloat16))
    hidden = jnp.concatenate(hidden_pieces, axis=2)
    picks = [
        (position[:, k][:, None] == slot_ids[None, :]).astype(jnp.bfloat16) for k in range(visits)
    ]
    moe_parts = []
    down_full = jnp.concatenate(down, axis=2)
    for down_piece in jnp.split(down_full, DOWN_PARTS, axis=1):
        results = jnp.einsum("xcf,xdf->xcd", hidden, down_piece, preferred_element_type=jnp.float32)
        from_other = swapped(results[:, rows:].astype(jnp.bfloat16), "tp")
        summed = (results[:, :rows] + from_other.astype(jnp.float32)).astype(jnp.bfloat16)
        summed = summed.reshape(local_experts, ep_size, capacity, -1).transpose(1, 0, 2, 3)
        returned = lax.all_to_all(summed, "ep", split_axis=0, concat_axis=0, tiled=True)
        flat_back = returned.reshape(experts * capacity, returned.shape[3])
        moe_parts.append(
            sum(
                route_weight[:, k][:, None]
                * jnp.dot(picks[k], flat_back, preferred_element_type=jnp.float32)
                for k in range(visits)
            )
        )
    moe = jnp.concatenate(moe_parts, axis=1)
    moe_output = scale_rows(moe, out_gain).astype(jnp.bfloat16)
    return (mixer_output, moe_output)


def solution(mesh):
    return jax.shard_map(
        per_device,
        mesh=mesh,
        in_specs=(
            P("ep", "tp"),
            P("ep", None),
            P("ep", None),
            P("tp"),
            P("tp"),
            P("tp", None),
            P(),
            P(("ep", "tp"), None),
            P(),
            P(),
            P(),
            P(),
            P(("ep", "tp"), None),
            P("ep", None, "tp"),
            P("ep", None, "tp"),
            P("ep", None, "tp"),
        ),
        out_specs=(P(("ep", "tp"), None), P(("ep", "tp"), None)),
        check_vma=False,
    )
```
